32 devices in a mesh: sp: 8 (over z, x), tp: 4 (over y, core).
Axes of the slice: x: 2, y: 2, z: 4, core: 2. Of those that a mesh axis runs over, the one named last changes fastest.
Arguments:
- query_proj: bfloat16 [4096, 1024], P('sp', 'tp'), may hold values from -6 to 6
- projected_keys: bfloat16 [4096, 512], P('sp', 'tp'), may hold values from -6 to 6
- projected_values: bfloat16 [4096, 512], P('sp', 'tp'), may hold values from -6 to 6
- residual: bfloat16 [4096, 2048], P(('sp', 'tp')), may hold values from -6 to 6
- out_weight: bfloat16 [1024, 2048], replicated, may hold values from -0.1875 to 0.1875
- mix_gain: float32 [2048], replicated, may hold values from 0.1 to 1.9
- norm_gain: float32 [2048], replicated, may hold values from 0.1 to 1.9
- route_expert: int32 [4096, 2], P(('sp', 'tp')), may hold values from 0 to 31, all different within a row; in each aligned block of 128 rows (0 to 127, 128 to 255, ...) at most 16 rows name the same one
- route_weight: float32 [4096, 2], P(('sp', 'tp')), may hold values from 0.2 to 1
- expert_gate: bfloat16 [32, 2048, 1024], P(('sp', 'tp')), may hold values from -0.125 to 0.125
- expert_up: bfloat16 [32, 2048, 1024], P(('sp', 'tp')), may hold values from -0.125 to 0.125
- expert_down: bfloat16 [32, 1024, 2048], P(('sp', 'tp')), may hold values from -0.1875 to 0.1875
Outputs:
- output: bfloat16 [4096, 2048], P(('sp', 'tp'))
The draws below stay inside these ranges and needn't reach their ends.
Inputs may be any that keep to these rules, and one draw needn't show every extreme that they name: `route_expert`: each row names 2 different experts. The rows of one device (aligned blocks of 128 rows) name any one expert at most 16 times, and in some blocks some expert is named exactly 16 times.
All inputs are finite; a program needn't handle non-finite values.
Results may differ from the reference program's by a relative error of at most 0.015.
Values may be sent and summed in bfloat16 or wider, within the bound.
A program may use at most 128 MiB of HBM per device.

```python
import math
import jax
import jax.numpy as jnp
import numpy as np
from jax import lax

D = 2048
QUERY_HEADS = 16
KEY_VALUE_HEADS = 8
HEAD_SIZE = 64
FF = 1024
TOP = 2
GRID_W = 64
ROWS = 128
SEQUENCE_TOKENS = 4096
EXPERTS = 32
CAP = 16
N_SP = 8
N_TP = 4


def block_levels(own_key, shape, cuts, low, top_value):
    def one(dim, shards_of):
        heights = jax.random.uniform(jax.random.fold_in(jax.random.fold_in(own_key, 6), dim), (shards_of,), jnp.float32, low / len(cuts), top_value / len(cuts))
        return jnp.repeat(jnp.exp(heights), shape[dim] // shards_of).reshape((-1,) + (1,) * (len(shape) - dim - 1))

    gain = one(*cuts[0])
    for cut in cuts[1:]:
        gain = gain * one(*cut)
    return gain


def deal_out(key, own, number, rows, count, top, bound, skew):
    ranking = jax.random.permutation(key, count)
    heavy_load, common = shares(count, rows * top, bound, skew, True), shares(count, rows * top, bound, skew, False)
    places = jnp.arange(count)

    def named(lengths, rotation):
        used = int((lengths > 0).sum())
        fixed = max(1, used // 4)
        moved = fixed + (places - fixed + rotation * (used - fixed)) % max(1, count - fixed)
        return jnp.zeros((count,), jnp.int32).at[ranking[jnp.where(places < fixed, places, moved)]].set(jnp.asarray(lengths, jnp.int32))

    lengths = jnp.where(number % 4 == 0, named(heavy_load, number // 4), named(common, number - number // 4 - 1))
    mixed = jax.random.permutation(jax.random.fold_in(own, 3), count)
    source_of, taker = mixed[0:count // 2 * 2:2], mixed[1:count // 2 * 2:2]
    margin = jnp.minimum(lengths[source_of] - 1, bound - lengths[taker]) // 2
    margin = jnp.where((source_of == ranking[0]) | (taker == ranking[0]) | (lengths[taker] == 0), 0, jnp.maximum(margin, 0))
    moved = jax.random.randint(jax.random.fold_in(own, 4), (count // 2,), 0, 1 << 20) % (margin + 1)
    lengths = lengths.at[source_of].add(-moved).at[taker].add(moved)
    labels = jnp.searchsorted(jnp.cumsum(lengths), jnp.arange(rows * top), side="right").astype(jnp.int32)
    grid = labels.reshape(top, rows).T
    grid = grid[jax.random.permutation(jax.random.fold_in(own, 1), rows)]
    rotation = jax.random.randint(jax.random.fold_in(own, 2), (rows, 1), 0, top)
    return jnp.take_along_axis(grid, (jnp.arange(top)[None, :] + rotation) % top, axis=1)


def shares(amount, total, reach, slope, full):
    weights = [(1 << 20) // math.isqrt(grade ** slope) + 1 for grade in range(1, amount + 1)]
    largest = reach if full else min(reach, max(-(-total // amount), total * weights[0] // sum(weights)))
    least = 1 if total - largest >= amount - 1 else 0
    given, spare = [largest] + [least] * (amount - 1), total - largest - least * (amount - 1)
    while spare > 0:
        candidates = [i for i in range(1, amount) if given[i] < largest] or [i for i in range(1, amount) if given[i] < reach]
        pool, budget = sum([weights[i] for i in candidates]), spare
        for i in candidates:
            more = min(reach - given[i], max(1, budget * weights[i] // pool), spare)
            given[i] = given[i] + more
            spare = spare - more
    return np.array(given)


def bell_draw(rng, dims, deviation, most, pieces=(), kind=jnp.bfloat16):
    entries = jax.random.normal(rng, dims, jnp.float32) * deviation
    if len(pieces) > 0:
        entries = block_levels(rng, dims, pieces, -0.22, 0.18) * entries
    return jnp.clip(entries, min=-most, max=most).astype(kind)


def setup_inputs(seed: int = 0) -> dict:
    key_list = jax.random.split(jax.random.key(seed), 13)
    query_proj = bell_draw(key_list[0], (SEQUENCE_TOKENS, QUERY_HEADS * HEAD_SIZE), 1.0, 6.0, ((0, 8), (1, 4)))
    projected_keys = bell_draw(key_list[1], (SEQUENCE_TOKENS, KEY_VALUE_HEADS * HEAD_SIZE), 1.0, 6.0, ((0, 8), (1, 4)))
    projected_values = bell_draw(key_list[2], (SEQUENCE_TOKENS, KEY_VALUE_HEADS * HEAD_SIZE), 1.0, 6.0, ((0, 8), (1, 4)))
    residual = bell_draw(key_list[3], (SEQUENCE_TOKENS, D), 1.0, 6.0, ((0, 32),))
    out_weight = bell_draw(key_list[4], (QUERY_HEADS * HEAD_SIZE, D), (QUERY_HEADS * HEAD_SIZE) ** -0.5, 0.1875)
    mix_gain = jnp.clip(1.0 + 0.18 * jax.random.normal(key_list[5], (D,), jnp.float32), 0.1, 1.9)
    norm_gain = jnp.clip(1.0 + 0.18 * jax.random.normal(key_list[6], (D,), jnp.float32), 0.1, 1.9)
    route_expert_keys = jax.random.split(jax.random.fold_in(key_list[7], 1), SEQUENCE_TOKENS // ROWS)
    route_expert_turns = jax.random.permutation(jax.random.fold_in(key_list[7], 3), SEQUENCE_TOKENS // ROWS)
    route_expert = jax.vmap(lambda own, number: deal_out(jax.random.fold_in(key_list[7], 2), own, number, ROWS, EXPERTS, TOP, CAP, 2))(route_expert_keys, route_expert_turns).reshape((SEQUENCE_TOKENS, TOP))
    route_weight = jnp.clip(0.2 + 0.8 * jax.random.uniform(key_list[8], (SEQUENCE_TOKENS, TOP), jnp.float32) ** block_levels(key_list[8], (SEQUENCE_TOKENS, TOP), ((0, 32),), -0.2, 0.2), 0.2, 1.0)
    expert_gate = bell_draw(key_list[9], (EXPERTS, D, FF), D ** -0.5, 0.125, ((0, 32),))
    expert_up = bell_draw(key_list[10], (EXPERTS, D, FF), D ** -0.5, 0.125, ((0, 32),))
    expert_down = bell_draw(key_list[11], (EXPERTS, FF, D), FF ** -0.5, 0.1875, ((0, 32),))
    return dict(query_proj=query_proj, projected_keys=projected_keys, projected_values=projected_values, residual=residual, out_weight=out_weight, mix_gain=mix_gain, norm_gain=norm_gain, route_expert=route_expert, route_weight=route_weight, expert_gate=expert_gate, expert_up=expert_up, expert_down=expert_down)


epsilon = 1e-06
base_theta = 10000.0

def unit_length_rows(values):
    values = values.astype(jnp.float32)
    return values * lax.rsqrt(lax.optimization_barrier(jnp.mean(values * values, axis=-1, keepdims=True)) + epsilon)

def rotary_embed(head_vecs, offset):
    row_count = head_vecs.shape[0]
    quarter = head_vecs.shape[-1] // 4
    places = offset + jnp.arange(row_count, dtype=jnp.int32)
    grid_row = (places // GRID_W).astype(jnp.float32)
    grid_col = (places % GRID_W).astype(jnp.float32)
    frequency = base_theta ** (-jnp.arange(quarter, dtype=jnp.float32) / quarter)
    row_angle = grid_row[:, None, None] * frequency
    col_angle = grid_col[:, None, None] * frequency
    row_cos, row_sin = (jnp.cos(row_angle), jnp.sin(row_angle))
    col_cos, col_sin = (jnp.cos(col_angle), jnp.sin(col_angle))
    row_first = head_vecs[..., :quarter]
    row_second = head_vecs[..., quarter:2 * quarter]
    col_first = head_vecs[..., 2 * quarter:3 * quarter]
    col_second = head_vecs[..., 3 * quarter:]
    return jnp.concatenate([row_first * row_cos - row_second * row_sin, row_second * row_cos + row_first * row_sin, col_first * col_cos - col_second * col_sin, col_second * col_cos + col_first * col_sin], axis=-1)

def reference(query_proj, projected_keys, projected_values, residual, out_weight, mix_gain, norm_gain, route_expert, route_weight, expert_gate, expert_up, expert_down):
    query_group = QUERY_HEADS // KEY_VALUE_HEADS
    query_prepared = rotary_embed(unit_length_rows(query_proj.reshape(SEQUENCE_TOKENS, QUERY_HEADS, HEAD_SIZE)), 0).astype(jnp.bfloat16)
    query_prepared = query_prepared.reshape(SEQUENCE_TOKENS, KEY_VALUE_HEADS, query_group, HEAD_SIZE)
    key_prepared = rotary_embed(unit_length_rows(projected_keys.reshape(SEQUENCE_TOKENS, KEY_VALUE_HEADS, HEAD_SIZE)), 0).astype(jnp.bfloat16)
    k_wide = key_prepared.astype(jnp.float32)
    value_broad = projected_values.reshape(SEQUENCE_TOKENS, KEY_VALUE_HEADS, HEAD_SIZE).astype(jnp.float32)
    scale = HEAD_SIZE ** (-0.5)
    model_width = math.gcd(SEQUENCE_TOKENS, 256)

    def attend(q_block):
        scores = jnp.einsum('thgd,nhd->thgn', q_block.astype(jnp.float32), k_wide) * scale
        weights = jnp.exp(scores)
        totals = lax.optimization_barrier(jnp.sum(weights, axis=-1))
        weights_low = lax.optimization_barrier(weights.astype(jnp.bfloat16))
        sums = jnp.einsum('thgn,nhd->thgd', weights_low.astype(jnp.float32), value_broad)
        return (sums / totals[..., None]).astype(jnp.bfloat16)
    block_list = query_prepared.reshape(SEQUENCE_TOKENS // model_width, model_width, KEY_VALUE_HEADS, query_group, HEAD_SIZE)
    attended = lax.map(attend, block_list).reshape(SEQUENCE_TOKENS, QUERY_HEADS * HEAD_SIZE)
    mixed = jnp.dot(attended, out_weight, preferred_element_type=jnp.float32)
    stream = (residual.astype(jnp.float32) + unit_length_rows(mixed) * mix_gain).astype(jnp.bfloat16)
    normed = (unit_length_rows(stream) * norm_gain).astype(jnp.bfloat16)
    limit = N_SP * N_TP * CAP
    flat_expert = route_expert.reshape(-1).astype(jnp.int32)
    order = jnp.argsort(flat_expert, stable=True).astype(jnp.int32)
    counts = lax.optimization_barrier(jnp.sum((flat_expert[:, None] == jnp.arange(EXPERTS, dtype=jnp.int32)[None, :]).astype(jnp.int32), axis=0))
    starts = (jnp.cumsum(counts) - counts).astype(jnp.int32)
    padded = jnp.concatenate([order, jnp.zeros((limit,), jnp.int32)])

    def one_expert(index):
        chosen = lax.dynamic_slice_in_dim(padded, starts[index], limit)
        rows_in = normed[chosen // TOP]
        gate_pre = jnp.dot(rows_in, expert_gate[index], preferred_element_type=jnp.float32)
        up_pre = jnp.dot(rows_in, expert_up[index], preferred_element_type=jnp.float32)
        expert_act = (jax.nn.silu(gate_pre) * up_pre).astype(jnp.bfloat16)
        return jnp.dot(expert_act, expert_down[index], preferred_element_type=jnp.float32).astype(jnp.bfloat16)
    results = lax.map(one_expert, jnp.arange(EXPERTS, dtype=jnp.int32))
    position = jnp.argsort(order, stable=True).astype(jnp.int32)
    rank = (position - starts[flat_expert]).astype(jnp.int32)
    picked = results[flat_expert, rank].reshape(SEQUENCE_TOKENS, TOP, D)
    combined = lax.optimization_barrier(jnp.sum(picked.astype(jnp.float32) * route_weight[:, :, None], axis=1))
    return (stream.astype(jnp.float32) + combined).astype(jnp.bfloat16)
```

```python
import functools
import math

import jax
import jax.numpy as jnp
from jax import lax
from jax.experimental import pallas as pl
from jax.experimental.pallas import tpu as pltpu
from jax.sharding import PartitionSpec as P

D = 2048
HEAD_SIZE = 64
GRID_W = 64


epsilon = 1e-06
base_theta = 10000.0


def unit_length_rows(values):
    values = values.astype(jnp.float32)
    return values * lax.rsqrt(jnp.mean(values * values, axis=-1, keepdims=True) + epsilon)


MESH = pl.DeviceIdType.MESH
LANES = 2 * HEAD_SIZE


def ring_step(sp, delta, n, nz, nx):
    z, x = sp // nx, sp % nx
    place = x * nz + z + (x % 2) * (nz - 1 - 2 * z)
    place = (place + delta + n) % n
    x = place // nz
    z = place % nz
    z = z + (x % 2) * (nz - 1 - 2 * z)
    return z * nx + x


def attend_kernel(
    n, nz, nx, ntp, group,
    q_ref, k_ref, v_ref, cos_ref, sin_ref, swap_ref, ones_ref,
    out_ref,
    qs, acc, fb, bb, att, rx,
    send_f, recv_f, send_b, recv_b, send_t, recv_t,
):
    sp = lax.axis_index("sp")
    tp = lax.axis_index("tp")
    toks = q_ref.shape[0]
    heads = q_ref.shape[1] // HEAD_SIZE
    half = toks // 2
    steps = n - 1
    nxt = ring_step(sp, 1, n, nz, nx)
    prv = ring_step(sp, -1, n, nz, nx)

    barrier = pltpu.get_barrier_semaphore()
    for other in (nxt, prv):
        pl.semaphore_signal(barrier, inc=1, device_id=(other, tp), device_id_type=MESH)
    for d in range(1, ntp):
        pl.semaphore_signal(
            barrier, inc=1, device_id=(sp, (tp + d) % ntp), device_id_type=MESH
        )

    cos = cos_ref[...]
    sin = sin_ref[...]
    low = lax.broadcasted_iota(jnp.int32, (toks, LANES), 1) < HEAD_SIZE

    def prepare(block):
        wide = block.astype(jnp.float32)
        square = wide * wide
        hi = square.astype(jnp.bfloat16)
        lo = (square - hi.astype(jnp.float32)).astype(jnp.bfloat16)
        mean = jnp.dot(hi, ones_ref[...], preferred_element_type=jnp.float32) + jnp.dot(
            lo, ones_ref[...], preferred_element_type=jnp.float32
        )
        partner = jnp.dot(block, swap_ref[...], preferred_element_type=jnp.float32)
        return (wide * cos + partner * sin) * lax.rsqrt(mean + epsilon)

    keys = prepare(k_ref[...]).astype(jnp.bfloat16)
    vals = v_ref[...]
    for c in range(2):
        rows = slice(c * half, (c + 1) * half)
        fb[c, 0] = keys[rows]
        fb[c, 1] = vals[rows]
        bb[1 - c, 0] = keys[rows]
        bb[1 - c, 1] = vals[rows]

    def forward(i):
        return pltpu.make_async_remote_copy(
            src_ref=fb.at[i], dst_ref=fb.at[i + 2],
            send_sem=send_f.at[i], recv_sem=recv_f.at[i],
            device_id=(nxt, tp), device_id_type=MESH,
        )

    def backward(i):
        return pltpu.make_async_remote_copy(
            src_ref=bb.at[i], dst_ref=bb.at[i + 2],
            send_sem=send_b.at[i], recv_sem=recv_b.at[i],
            device_id=(prv, tp), device_id_type=MESH,
        )

    pl.semaphore_wait(barrier, 2 + ntp - 1)
    for i in range(2):
        forward(i).start()
        backward(i).start()

    scale = HEAD_SIZE ** (-0.5)
    for t in range(heads // 2):
        ready = prepare(q_ref[:, t * LANES : (t + 1) * LANES]) * scale
        for h in (2 * t, 2 * t + 1):
            side = (h // group) % 2
            lined = ready if h % 2 == side else pltpu.roll(ready, HEAD_SIZE, 1)
            keep = low if side == 0 else jnp.logical_not(low)
            qs[h * toks : (h + 1) * toks] = jnp.where(keep, lined, 0.0).astype(jnp.bfloat16)
    acc[...] = jnp.zeros_like(acc)
    tile = math.gcd(toks, 256)
    vlow = lax.broadcasted_iota(jnp.int32, (toks, LANES), 1) < HEAD_SIZE

    def one_step(j, carry):
        at = j + jnp.minimum(j, 1)

        @pl.when(j > 0)
        def _():
            forward(j - 1).wait_recv()
            backward(j - 1).wait_recv()

        @pl.when(jnp.logical_and(j > 0, j + 1 < steps))
        def _():
            forward(j + 1).start()
            backward(j + 1).start()

        kk = jnp.concatenate([fb[at, 0], bb[at, 0]], axis=0)
        vv = jnp.concatenate([fb[at, 1], bb[at, 1]], axis=0).astype(jnp.float32)
        sided = (
            jnp.where(vlow, vv, 1.0).astype(jnp.bfloat16),
            jnp.where(vlow, 1.0, vv).astype(jnp.bfloat16),
        )
        for h in range(heads):
            for r in range(toks // tile):
                rows = slice(h * toks + r * tile, h * toks + (r + 1) * tile)
                scores = lax.dot_general(
                    qs[rows], kk, (((1,), (1,)), ((), ())),
                    preferred_element_type=jnp.float32,
                )
                weights = jnp.exp(scores).astype(jnp.bfloat16)
                acc[rows] += jnp.dot(
                    weights, sided[(h // group) % 2], preferred_element_type=jnp.float32
                )
        return carry

    lax.fori_loop(0, steps + 1, one_step, 0)

    share = toks // ntp
    for t in range(heads // 2):
        parts = []
        for h in (2 * t, 2 * t + 1):
            mine = acc[h * toks : (h + 1) * toks]
            turned = pltpu.roll(mine, HEAD_SIZE, 1)
            parts.append(mine / turned if h % 2 == (h // group) % 2 else turned / mine)
        done = jnp.where(low, parts[0], parts[1]).astype(jnp.bfloat16)
        for p in range(ntp):
            att[p, :, t * LANES : (t + 1) * LANES] = done[p * share : (p + 1) * share]

    def across(d):
        to = (tp + d) % ntp
        return pltpu.make_async_remote_copy(
            src_ref=att.at[to], dst_ref=rx.at[tp],
            send_sem=send_t.at[d], recv_sem=recv_t.at[d],
            device_id=(sp, to), device_id_type=MESH,
        )

    for d in range(1, ntp):
        across(d).start()
    rx[tp] = att[tp]
    for i in range(steps):
        forward(i).wait_send()
        backward(i).wait_send()
    for d in range(1, ntp):
        across(d).wait_recv()
    width = q_ref.shape[1]
    for p in range(ntp):
        out_ref[:, p * width : (p + 1) * width] = rx[p]
    for d in range(1, ntp):
        across(d).wait_send()


def ring_sizes(mesh, n):
    try:
        coords = [tuple(d.coords) for d in mesh.devices[:, 0]]
        nz = len({c[2] for c in coords})
        nx = len({c[0] for c in coords})
        if nz * nx == n and nz > 1:
            return nz, nx
    except Exception:
        pass
    return n, 1


def attend(mesh, query_proj, projected_keys, projected_values):
    n, ntp = mesh.shape["sp"], mesh.shape["tp"]
    nz, nx = ring_sizes(mesh, n)
    toks, width = query_proj.shape
    heads = width // HEAD_SIZE
    group = heads // (projected_keys.shape[1] // HEAD_SIZE)
    spare = LANES - projected_keys.shape[1]
    if spare:
        projected_keys = jnp.pad(projected_keys, ((0, 0), (0, spare)))
        projected_values = jnp.pad(projected_values, ((0, 0), (0, spare)))
    quarter = HEAD_SIZE // 4
    places = lax.axis_index("sp") * toks + jnp.arange(toks, dtype=jnp.int32)
    frequency = base_theta ** (-jnp.arange(quarter, dtype=jnp.float32) / quarter)
    lane = jnp.arange(LANES, dtype=jnp.int32)
    on_row = (lane % HEAD_SIZE) < 2 * quarter
    spot = jnp.where(on_row[None, :], (places // GRID_W)[:, None], (places % GRID_W)[:, None])
    angle = spot.astype(jnp.float32) * jnp.tile(frequency, LANES // quarter)[None, :]
    first = (lane // quarter) % 2 == 0
    source = jnp.where(first, lane + quarter, lane - quarter)
    swap = jnp.where(
        lane[:, None] == source[None, :], jnp.where(first, -1.0, 1.0)[None, :], 0.0
    ).astype(jnp.bfloat16)
    ones = jnp.where(
        lane[:, None] // HEAD_SIZE == lane[None, :] // HEAD_SIZE, 1.0 / HEAD_SIZE, 0.0
    ).astype(jnp.bfloat16)
    share = toks // ntp
    dma = pltpu.SemaphoreType.DMA
    return pl.pallas_call(
        functools.partial(attend_kernel, n, nz, nx, ntp, group),
        out_shape=jax.ShapeDtypeStruct((share, ntp * width), jnp.bfloat16),
        in_specs=[pl.BlockSpec(memory_space=pltpu.VMEM)] * 7,
        out_specs=pl.BlockSpec(memory_space=pltpu.VMEM),
        scratch_shapes=[
            pltpu.VMEM((heads * toks, LANES), jnp.bfloat16),
            pltpu.VMEM((heads * toks, LANES), jnp.float32),
            pltpu.VMEM((n + 1, 2, toks // 2, LANES), jnp.bfloat16),
            pltpu.VMEM((n + 1, 2, toks // 2, LANES), jnp.bfloat16),
            pltpu.VMEM((ntp, share, width), jnp.bfloat16),
            pltpu.VMEM((ntp, share, width), jnp.bfloat16),
            dma((n - 1,)), dma((n - 1,)), dma((n - 1,)), dma((n - 1,)),
            dma((ntp,)), dma((ntp,)),
        ],
        compiler_params=pltpu.CompilerParams(
            collective_id=0, has_side_effects=True, vmem_limit_bytes=40 << 20
        ),
        name="attend",
    )(query_proj, projected_keys, projected_values, jnp.cos(angle), jnp.sin(angle), swap, ones)


def local(
    mesh,
    query_proj,
    projected_keys,
    projected_values,
    residual,
    out_weight,
    mix_gain,
    norm_gain,
    route_expert,
    route_weight,
    expert_gate,
    expert_up,
    expert_down,
):
    by_token = attend(mesh, query_proj, projected_keys, projected_values)
    mixed = jnp.dot(by_token, out_weight, preferred_element_type=jnp.float32)
    stream = (residual.astype(jnp.float32) + unit_length_rows(mixed) * mix_gain).astype(
        jnp.bfloat16
    )
    normed = (unit_length_rows(stream) * norm_gain).astype(jnp.bfloat16)
    row_count = normed.shape[0]
    top_count = route_expert.shape[1]
    experts = lax.axis_size("sp") * lax.axis_size("tp")
    capacity = max(2, 2 * top_count * row_count // experts)
    flat_expert = route_expert.reshape(-1)
    onehot = (flat_expert[:, None] == jnp.arange(experts, dtype=jnp.int32)[None, :]).astype(
        jnp.int32
    )
    earlier = jnp.cumsum(onehot, axis=0) - onehot
    slot_rank = jnp.sum(earlier * onehot, axis=1)
    target = flat_expert * capacity + slot_rank
    placing = jnp.arange(experts * capacity, dtype=jnp.int32)[:, None] == target[None, :]
    placing = jnp.any(placing.reshape(experts * capacity, row_count, top_count), axis=2).astype(
        jnp.bfloat16
    )
    outgoing = jnp.dot(placing, normed, preferred_element_type=jnp.float32).astype(jnp.bfloat16)
    outgoing = outgoing.reshape(experts, capacity, D)
    gate_mat = expert_gate[0]
    up_mat = expert_up[0]
    down_mat = expert_down[0]
    slots = lax.all_to_all(outgoing, ("sp", "tp"), split_axis=0, concat_axis=0, tiled=True)
    flat_rows = slots.reshape(-1, slots.shape[-1])
    gate_pre = jnp.dot(flat_rows, gate_mat, preferred_element_type=jnp.float32)
    up_pre = jnp.dot(flat_rows, up_mat, preferred_element_type=jnp.float32)
    expert_act = (jax.nn.silu(gate_pre) * up_pre).astype(jnp.bfloat16)
    done = jnp.dot(expert_act, down_mat, preferred_element_type=jnp.float32).astype(jnp.bfloat16)
    answered = done.reshape(slots.shape)
    returned = lax.all_to_all(answered, ("sp", "tp"), split_axis=0, concat_axis=0, tiled=True)
    picked = jnp.take(returned.reshape(experts * capacity, D), target, axis=0).reshape(
        row_count, top_count, D
    )
    combined = jnp.sum(picked.astype(jnp.float32) * route_weight[:, :, None], axis=1)
    return (stream.astype(jnp.float32) + combined).astype(jnp.bfloat16)


def solution(mesh):
    return jax.shard_map(
        functools.partial(local, mesh),
        mesh=mesh,
        in_specs=(
            P("sp", "tp"),
            P("sp", "tp"),
            P("sp", "tp"),
            P(("sp", "tp"), None),
            P(),
            P(),
            P(),
            P(("sp", "tp"), None),
            P(("sp", "tp"), None),
            P(("sp", "tp"), None, None),
            P(("sp", "tp"), None, None),
            P(("sp", "tp"), None, None),
        ),
        out_specs=P(("sp", "tp"), None),
        check_vma=False,
    )
```

```python
import functools
import math

import jax
import jax.numpy as jnp
from jax import lax
from jax.experimental import pallas as pl
from jax.experimental.pallas import tpu as pltpu
from jax.sharding import PartitionSpec as P

D = 2048
HEAD_SIZE = 64
GRID_W = 64


epsilon = 1e-06
base_theta = 10000.0


def unit_length_rows(values):
    values = values.astype(jnp.float32)
    return values * lax.rsqrt(jnp.mean(values * values, axis=-1, keepdims=True) + epsilon)


MESH = pl.DeviceIdType.MESH
LANES = 2 * HEAD_SIZE


def ring_step(sp, delta, n, nz, nx):
    z, x = sp // nx, sp % nx
    place = x * nz + z + (x % 2) * (nz - 1 - 2 * z)
    place = (place + delta + n) % n
    x = place // nz
    z = place % nz
    z = z + (x % 2) * (nz - 1 - 2 * z)
    return z * nx + x


def attend_kernel(
    n, nz, nx, ntp, group,
    q_ref, k_ref, v_ref, cos_ref, sin_ref, swap_ref, ones_ref,
    out_ref,
    qs, acc, fb, bb, att, rx,
    send_f, recv_f, send_b, recv_b, send_t, recv_t,
):
    sp = lax.axis_index("sp")
    tp = lax.axis_index("tp")
    toks = q_ref.shape[0]
    heads = q_ref.shape[1] // HEAD_SIZE
    half = toks // 2
    steps = n - 1
    nxt = ring_step(sp, 1, n, nz, nx)
    prv = ring_step(sp, -1, n, nz, nx)

    barrier = pltpu.get_barrier_semaphore()
    for other in (nxt, prv):
        pl.semaphore_signal(barrier, inc=1, device_id=(other, tp), device_id_type=MESH)
    for d in range(1, ntp):
        pl.semaphore_signal(
            barrier, inc=1, device_id=(sp, (tp + d) % ntp), device_id_type=MESH
        )

    cos = cos_ref[...]
    sin = sin_ref[...]
    low = lax.broadcasted_iota(jnp.int32, (toks, LANES), 1) < HEAD_SIZE

    def prepare(block):
        wide = block.astype(jnp.float32)
        square = wide * wide
        hi = square.astype(jnp.bfloat16)
        lo = (square - hi.astype(jnp.float32)).astype(jnp.bfloat16)
        mean = jnp.dot(hi, ones_ref[...], preferred_element_type=jnp.float32) + jnp.dot(
            lo, ones_ref[...], preferred_element_type=jnp.float32
        )
        partner = jnp.dot(block, swap_ref[...], preferred_element_type=jnp.float32)
        return (wide * cos + partner * sin) * lax.rsqrt(mean + epsilon)

    keys = prepare(k_ref[...]).astype(jnp.bfloat16)
    vals = v_ref[...]
    for c in range(2):
        rows = slice(c * half, (c + 1) * half)
        fb[c, 0] = keys[rows]
        fb[c, 1] = vals[rows]
        bb[1 - c, 0] = keys[rows]
        bb[1 - c, 1] = vals[rows]

    def forward(i):
        return pltpu.make_async_remote_copy(
            src_ref=fb.at[i], dst_ref=fb.at[i + 2],
            send_sem=send_f.at[i], recv_sem=recv_f.at[i],
            device_id=(nxt, tp), device_id_type=MESH,
        )

    def backward(i):
        return pltpu.make_async_remote_copy(
            src_ref=bb.at[i], dst_ref=bb.at[i + 2],
            send_sem=send_b.at[i], recv_sem=recv_b.at[i],
            device_id=(prv, tp), device_id_type=MESH,
        )

    pl.semaphore_wait(barrier, 2 + ntp - 1)
    for i in range(2):
        forward(i).start()
        backward(i).start()

    scale = HEAD_SIZE ** (-0.5)
    for t in range(heads // 2):
        ready = prepare(q_ref[:, t * LANES : (t + 1) * LANES]) * scale
        for h in (2 * t, 2 * t + 1):
            side = (h // group) % 2
            lined = ready if h % 2 == side else pltpu.roll(ready, HEAD_SIZE, 1)
            keep = low if side == 0 else jnp.logical_not(low)
            qs[h * toks : (h + 1) * toks] = jnp.where(keep, lined, 0.0).astype(jnp.bfloat16)
    acc[...] = jnp.zeros_like(acc)
    tile = math.gcd(toks, 256)
    vlow = lax.broadcasted_iota(jnp.int32, (toks, LANES), 1) < HEAD_SIZE

    def one_step(j, carry):
        at = j + jnp.minimum(j, 1)

        @pl.when(j > 0)
        def _():
            forward(j - 1).wait_recv()
            backward(j - 1).wait_recv()

        @pl.when(jnp.logical_and(j > 0, j + 1 < steps))
        def _():
            forward(j + 1).start()
            backward(j + 1).start()

        kk = jnp.concatenate([fb[at, 0], bb[at, 0]], axis=0)
        vv = jnp.concatenate([fb[at, 1], bb[at, 1]], axis=0).astype(jnp.float32)
        sided = (
            jnp.where(vlow, vv, 1.0).astype(jnp.bfloat16),
            jnp.where(vlow, 1.0, vv).astype(jnp.bfloat16),
        )
        for h in range(heads):
            for r in range(toks // tile):
                rows = slice(h * toks + r * tile, h * toks + (r + 1) * tile)
                scores = lax.dot_general(
                    qs[rows], kk, (((1,), (1,)), ((), ())),
                    preferred_element_type=jnp.float32,
                )
                weights = jnp.exp(scores).astype(jnp.bfloat16)
                acc[rows] += jnp.dot(
                    weights, sided[(h // group) % 2], preferred_element_type=jnp.float32
                )
        return carry

    lax.fori_loop(0, steps + 1, one_step, 0)

    share = toks // ntp
    for t in range(heads // 2):
        parts = []
        for h in (2 * t, 2 * t + 1):
            mine = acc[h * toks : (h + 1) * toks]
            turned = pltpu.roll(mine, HEAD_SIZE, 1)
            parts.append(mine / turned if h % 2 == (h // group) % 2 else turned / mine)
        done = jnp.where(low, parts[0], parts[1]).astype(jnp.bfloat16)
        for p in range(ntp):
            att[p, :, t * LANES : (t + 1) * LANES] = done[p * share : (p + 1) * share]

    def across(d):
        to = (tp + d) % ntp
        return pltpu.make_async_remote_copy(
            src_ref=att.at[to], dst_ref=rx.at[tp],
            send_sem=send_t.at[d], recv_sem=recv_t.at[d],
            device_id=(sp, to), device_id_type=MESH,
        )

    for d in range(1, ntp):
        across(d).start()
    rx[tp] = att[tp]
    for i in range(steps):
        forward(i).wait_send()
        backward(i).wait_send()
    for d in range(1, ntp):
        across(d).wait_recv()
    width = q_ref.shape[1]
    for p in range(ntp):
        out_ref[:, p * width : (p + 1) * width] = rx[p]
    for d in range(1, ntp):
        across(d).wait_send()


def ring_sizes(mesh, n):
    try:
        coords = [tuple(d.coords) for d in mesh.devices[:, 0]]
        nz = len({c[2] for c in coords})
        nx = len({c[0] for c in coords})
        if nz * nx == n and nz > 1:
            return nz, nx
    except Exception:
        pass
    return n, 1


def attend(mesh, query_proj, projected_keys, projected_values):
    n, ntp = mesh.shape["sp"], mesh.shape["tp"]
    nz, nx = ring_sizes(mesh, n)
    toks, width = query_proj.shape
    heads = width // HEAD_SIZE
    group = heads // (projected_keys.shape[1] // HEAD_SIZE)
    spare = LANES - projected_keys.shape[1]
    if spare:
        projected_keys = jnp.pad(projected_keys, ((0, 0), (0, spare)))
        projected_values = jnp.pad(projected_values, ((0, 0), (0, spare)))
    quarter = HEAD_SIZE // 4
    places = lax.axis_index("sp") * toks + jnp.arange(toks, dtype=jnp.int32)
    frequency = base_theta ** (-jnp.arange(quarter, dtype=jnp.float32) / quarter)
    lane = jnp.arange(LANES, dtype=jnp.int32)
    on_row = (lane % HEAD_SIZE) < 2 * quarter
    spot = jnp.where(on_row[None, :], (places // GRID_W)[:, None], (places % GRID_W)[:, None])
    angle = spot.astype(jnp.float32) * jnp.tile(frequency, LANES // quarter)[None, :]
    first = (lane // quarter) % 2 == 0
    source = jnp.where(first, lane + quarter, lane - quarter)
    swap = jnp.where(
        lane[:, None] == source[None, :], jnp.where(first, -1.0, 1.0)[None, :], 0.0
    ).astype(jnp.bfloat16)
    ones = jnp.where(
        lane[:, None] // HEAD_SIZE == lane[None, :] // HEAD_SIZE, 1.0 / HEAD_SIZE, 0.0
    ).astype(jnp.bfloat16)
    share = toks // ntp
    dma = pltpu.SemaphoreType.DMA
    return pl.pallas_call(
        functools.partial(attend_kernel, n, nz, nx, ntp, group),
        out_shape=jax.ShapeDtypeStruct((share, ntp * width), jnp.bfloat16),
        in_specs=[pl.BlockSpec(memory_space=pltpu.VMEM)] * 7,
        out_specs=pl.BlockSpec(memory_space=pltpu.VMEM),
        scratch_shapes=[
            pltpu.VMEM((heads * toks, LANES), jnp.bfloat16),
            pltpu.VMEM((heads * toks, LANES), jnp.float32),
            pltpu.VMEM((n + 1, 2, toks // 2, LANES), jnp.bfloat16),
            pltpu.VMEM((n + 1, 2, toks // 2, LANES), jnp.bfloat16),
            pltpu.VMEM((ntp, share, width), jnp.bfloat16),
            pltpu.VMEM((ntp, share, width), jnp.bfloat16),
            dma((n - 1,)), dma((n - 1,)), dma((n - 1,)), dma((n - 1,)),
            dma((ntp,)), dma((ntp,)),
        ],
        compiler_params=pltpu.CompilerParams(
            collective_id=0, has_side_effects=True, vmem_limit_bytes=40 << 20
        ),
        name="attend",
    )(query_proj, projected_keys, projected_values, jnp.cos(angle), jnp.sin(angle), swap, ones)


def moe_kernel(
    count, ntp, cap,
    tx, stream, pick, share_w, gate_hbm, up_hbm, down_hbm,
    out_ref,
    rx, res, ret, act, gate, up, down,
    send_o, recv_o, send_r, recv_r, wsem,
):
    me = lax.axis_index("sp") * ntp + lax.axis_index("tp")
    per = count // 4
    order = (2, 1, 3, 0)

    def device(offset):
        other = (me + offset + count) % count
        return (other // ntp, other % ntp)

    def block(d):
        return pl.ds(pl.multiple_of(d * cap, cap), cap)

    def dispatch(d):
        return pltpu.make_async_remote_copy(
            src_ref=tx.at[block(d)], dst_ref=rx.at[block(d)],
            send_sem=send_o.at[d], recv_sem=recv_o.at[d],
            device_id=device(d), device_id_type=MESH,
        )

    def answer(d):
        return pltpu.make_async_remote_copy(
            src_ref=res.at[block(d)], dst_ref=ret.at[block(d)],
            send_sem=send_r.at[d], recv_sem=recv_r.at[d],
            device_id=device(-d), device_id_type=MESH,
        )

    def each(first, last, action):
        def body(d, carry):
            action(d)
            return carry

        lax.fori_loop(max(first, 1), last, body, 0)

    barrier = pltpu.get_barrier_semaphore()
    each(1, count, lambda d: pl.semaphore_signal(
        barrier, inc=1, device_id=device(d), device_id_type=MESH
    ))
    loads = [
        pltpu.make_async_copy(gate_hbm.at[0], gate, wsem.at[0]),
        pltpu.make_async_copy(up_hbm.at[0], up, wsem.at[1]),
        pltpu.make_async_copy(down_hbm.at[0], down, wsem.at[2]),
    ]
    pl.semaphore_wait(barrier, count - 1)
    for g in order:
        each(g * per, (g + 1) * per, lambda d: dispatch(d).start())
    for load in loads:
        load.start()
    rx[0:cap] = tx[0:cap]

    def columns(total, body):
        tile = math.gcd(total, 256)

        def one(c, carry):
            body(pl.ds(pl.multiple_of(c * tile, tile), tile))
            return carry

        lax.fori_loop(0, total // tile, one, 0)

    for number, g in enumerate(order):
        each(g * per, (g + 1) * per, lambda d: dispatch(d).wait_recv())
        if number == 0:
            for load in loads:
                load.wait()
        rows = slice(g * per * cap, (g + 1) * per * cap)

        def hidden(cols):
            taken = rx[rows]
            pre = jnp.dot(taken, gate[:, cols], preferred_element_type=jnp.float32)
            lift = jnp.dot(taken, up[:, cols], preferred_element_type=jnp.float32)
            act[:, cols] = (pre / (1.0 + jnp.exp(-pre)) * lift).astype(jnp.bfloat16)

        def project(cols):
            res[rows, cols] = jnp.dot(
                act[...], down[:, cols], preferred_element_type=jnp.float32
            ).astype(jnp.bfloat16)

        columns(gate.shape[1], hidden)
        columns(down.shape[1], project)
        each(g * per, (g + 1) * per, lambda d: answer(d).start())
    ret[0:cap] = res[0:cap]
    each(1, count, lambda d: answer(d).wait_recv())

    def combine(cols):
        total = jnp.zeros((out_ref.shape[0], math.gcd(out_ref.shape[1], 256)), jnp.float32)
        for k in range(pick.shape[0]):
            total += share_w[:, k : k + 1] * jnp.dot(
                pick[k], ret[:, cols], preferred_element_type=jnp.float32
            )
        out_ref[:, cols] = (stream[:, cols].astype(jnp.float32) + total).astype(jnp.bfloat16)

    columns(out_ref.shape[1], combine)
    each(1, count, lambda d: dispatch(d).wait_send())
    each(1, count, lambda d: answer(d).wait_send())


def moe(mesh, cap, outgoing, stream, pick, share_w, expert_gate, expert_up, expert_down):
    ntp = mesh.shape["tp"]
    count = mesh.shape["sp"] * ntp
    width = outgoing.shape[1]
    ff = expert_gate.shape[2]
    dma = pltpu.SemaphoreType.DMA
    low = jnp.bfloat16
    return pl.pallas_call(
        functools.partial(moe_kernel, count, ntp, cap),
        out_shape=jax.ShapeDtypeStruct(stream.shape, low),
        in_specs=[pl.BlockSpec(memory_space=pltpu.VMEM)] * 4
        + [pl.BlockSpec(memory_space=pl.ANY)] * 3,
        out_specs=pl.BlockSpec(memory_space=pltpu.VMEM),
        scratch_shapes=[
            pltpu.VMEM((count * cap, width), low),
            pltpu.VMEM((count * cap, width), low),
            pltpu.VMEM((count * cap, width), low),
            pltpu.VMEM((count // 4 * cap, ff), low),
            pltpu.VMEM((width, ff), low),
            pltpu.VMEM((width, ff), low),
            pltpu.VMEM((ff, width), low),
            dma((count,)), dma((count,)), dma((count,)), dma((count,)), dma((3,)),
        ],
        compiler_params=pltpu.CompilerParams(
            collective_id=1, has_side_effects=True, vmem_limit_bytes=60 << 20
        ),
        name="moe",
    )(outgoing, stream, pick, share_w, expert_gate, expert_up, expert_down)


def local(
    mesh,
    query_proj,
    projected_keys,
    projected_values,
    residual,
    out_weight,
    mix_gain,
    norm_gain,
    route_expert,
    route_weight,
    expert_gate,
    expert_up,
    expert_down,
):
    by_token = attend(mesh, query_proj, projected_keys, projected_values)
    mixed = jnp.dot(by_token, out_weight, preferred_element_type=jnp.float32)
    stream = (residual.astype(jnp.float32) + unit_length_rows(mixed) * mix_gain).astype(
        jnp.bfloat16
    )
    normed = (unit_length_rows(stream) * norm_gain).astype(jnp.bfloat16)
    row_count = normed.shape[0]
    top_count = route_expert.shape[1]
    experts = lax.axis_size("sp") * lax.axis_size("tp")
    capacity = -(-max(2, 2 * top_count * row_count // experts) // 16) * 16
    flat_expert = route_expert.reshape(-1)
    onehot = (flat_expert[:, None] == jnp.arange(experts, dtype=jnp.int32)[None, :]).astype(
        jnp.int32
    )
    earlier = jnp.cumsum(onehot, axis=0) - onehot
    slot_rank = jnp.sum(earlier * onehot, axis=1)
    me = lax.axis_index("sp") * lax.axis_size("tp") + lax.axis_index("tp")
    target = ((flat_expert - me + experts) % experts) * capacity + slot_rank
    placing = jnp.arange(experts * capacity, dtype=jnp.int32)[:, None] == target[None, :]
    placing = jnp.any(placing.reshape(experts * capacity, row_count, top_count), axis=2).astype(
        jnp.bfloat16
    )
    outgoing = jnp.dot(placing, normed, preferred_element_type=jnp.float32).astype(jnp.bfloat16)
    places = jnp.arange(experts * capacity, dtype=jnp.int32)
    pick = target.reshape(row_count, top_count).T[:, :, None] == places
    return moe(
        mesh, capacity, outgoing, stream, pick.astype(jnp.bfloat16), route_weight,
        expert_gate, expert_up, expert_down,
    )


def solution(mesh):
    return jax.shard_map(
        functools.partial(local, mesh),
        mesh=mesh,
        in_specs=(
            P("sp", "tp"),
            P("sp", "tp"),
            P("sp", "tp"),
            P(("sp", "tp"), None),
            P(),
            P(),
            P(),
            P(("sp", "tp"), None),
            P(("sp", "tp"), None),
            P(("sp", "tp"), None, None),
            P(("sp", "tp"), None, None),
            P(("sp", "tp"), None, None),
        ),
        out_specs=P(("sp", "tp"), None),
        check_vma=False,
    )
```

```python
import functools
import math

import jax
import jax.numpy as jnp
from jax import lax
from jax.experimental import pallas as pl
from jax.experimental.pallas import tpu as pltpu
from jax.sharding import PartitionSpec as P

D = 2048
HEAD_SIZE = 64
GRID_W = 64


epsilon = 1e-06
base_theta = 10000.0


def unit_length_rows(values):
    values = values.astype(jnp.float32)
    return values * lax.rsqrt(jnp.mean(values * values, axis=-1, keepdims=True) + epsilon)


MESH = pl.DeviceIdType.MESH
LANES = 2 * HEAD_SIZE


def ring_step(sp, delta, n, nz, nx):
    z, x = sp // nx, sp % nx
    place = x * nz + z + (x % 2) * (nz - 1 - 2 * z)
    place = (place + delta + n) % n
    x = place // nz
    z = place % nz
    z = z + (x % 2) * (nz - 1 - 2 * z)
    return z * nx + x


def attend_kernel(
    n, nz, nx, ntp, group,
    q_hbm, k_hbm, v_hbm, cos_ref, sin_ref, swap_ref, ones_ref,
    out_ref,
    q_ref, k_ref, v_ref, qs, acc, fb, bb, att, rx,
    load_sem, send_f, recv_f, send_b, recv_b, send_t, recv_t,
):
    sp = lax.axis_index("sp")
    tp = lax.axis_index("tp")
    loads = [
        pltpu.make_async_copy(k_hbm, k_ref, load_sem.at[0]),
        pltpu.make_async_copy(v_hbm, v_ref, load_sem.at[1]),
        pltpu.make_async_copy(q_hbm, q_ref, load_sem.at[2]),
    ]
    for load in loads:
        load.start()
    toks = q_ref.shape[0]
    heads = q_ref.shape[1] // HEAD_SIZE
    half = toks // 2
    steps = n - 1
    nxt = ring_step(sp, 1, n, nz, nx)
    prv = ring_step(sp, -1, n, nz, nx)

    barrier = pltpu.get_barrier_semaphore()
    for other in (nxt, prv):
        pl.semaphore_signal(barrier, inc=1, device_id=(other, tp), device_id_type=MESH)
    for d in range(1, ntp):
        pl.semaphore_signal(
            barrier, inc=1, device_id=(sp, (tp + d) % ntp), device_id_type=MESH
        )

    cos = cos_ref[...]
    sin = sin_ref[...]
    low = lax.broadcasted_iota(jnp.int32, (toks, LANES), 1) < HEAD_SIZE

    def prepare(block):
        wide = block.astype(jnp.float32)
        square = wide * wide
        hi = square.astype(jnp.bfloat16)
        lo = (square - hi.astype(jnp.float32)).astype(jnp.bfloat16)
        mean = jnp.dot(hi, ones_ref[...], preferred_element_type=jnp.float32) + jnp.dot(
            lo, ones_ref[...], preferred_element_type=jnp.float32
        )
        partner = jnp.dot(block, swap_ref[...], preferred_element_type=jnp.float32)
        return (wide * cos + partner * sin) * lax.rsqrt(mean + epsilon)

    loads[0].wait()
    loads[1].wait()
    keys = prepare(k_ref[...]).astype(jnp.bfloat16)
    vals = v_ref[...]
    for c in range(2):
        rows = slice(c * half, (c + 1) * half)
        fb[c, 0] = keys[rows]
        fb[c, 1] = vals[rows]
        bb[1 - c, 0] = keys[rows]
        bb[1 - c, 1] = vals[rows]

    def forward(i):
        return pltpu.make_async_remote_copy(
            src_ref=fb.at[i], dst_ref=fb.at[i + 2],
            send_sem=send_f.at[i], recv_sem=recv_f.at[i],
            device_id=(nxt, tp), device_id_type=MESH,
        )

    def backward(i):
        return pltpu.make_async_remote_copy(
            src_ref=bb.at[i], dst_ref=bb.at[i + 2],
            send_sem=send_b.at[i], recv_sem=recv_b.at[i],
            device_id=(prv, tp), device_id_type=MESH,
        )

    pl.semaphore_wait(barrier, 2 + ntp - 1)
    for i in range(2):
        forward(i).start()
        backward(i).start()

    loads[2].wait()
    scale = HEAD_SIZE ** (-0.5)
    for t in range(heads // 2):
        ready = prepare(q_ref[:, t * LANES : (t + 1) * LANES]) * scale
        for h in (2 * t, 2 * t + 1):
            side = (h // group) % 2
            lined = ready if h % 2 == side else pltpu.roll(ready, HEAD_SIZE, 1)
            keep = low if side == 0 else jnp.logical_not(low)
            qs[h * toks : (h + 1) * toks] = jnp.where(keep, lined, 0.0).astype(jnp.bfloat16)
    acc[...] = jnp.zeros_like(acc)
    tile = math.gcd(toks, 256)
    vlow = lax.broadcasted_iota(jnp.int32, (toks, LANES), 1) < HEAD_SIZE

    def one_step(j, carry):
        at = j + jnp.minimum(j, 1)

        @pl.when(j > 0)
        def _():
            forward(j - 1).wait_recv()
            backward(j - 1).wait_recv()

        @pl.when(jnp.logical_and(j > 0, j + 1 < steps))
        def _():
            forward(j + 1).start()
            backward(j + 1).start()

        kk = jnp.concatenate([fb[at, 0], bb[at, 0]], axis=0)
        vv = jnp.concatenate([fb[at, 1], bb[at, 1]], axis=0).astype(jnp.float32)
        sided = (
            jnp.where(vlow, vv, 1.0).astype(jnp.bfloat16),
            jnp.where(vlow, 1.0, vv).astype(jnp.bfloat16),
        )
        for h in range(heads):
            for r in range(toks // tile):
                rows = slice(h * toks + r * tile, h * toks + (r + 1) * tile)
                scores = lax.dot_general(
                    qs[rows], kk, (((1,), (1,)), ((), ())),
                    preferred_element_type=jnp.float32,
                )
                weights = jnp.exp(scores).astype(jnp.bfloat16)
                acc[rows] += jnp.dot(
                    weights, sided[(h // group) % 2], preferred_element_type=jnp.float32
                )
        return carry

    lax.fori_loop(0, steps + 1, one_step, 0)

    share = toks // ntp
    for t in range(heads // 2):
        parts = []
        for h in (2 * t, 2 * t + 1):
            mine = acc[h * toks : (h + 1) * toks]
            turned = pltpu.roll(mine, HEAD_SIZE, 1)
            parts.append(mine / turned if h % 2 == (h // group) % 2 else turned / mine)
        done = jnp.where(low, parts[0], parts[1]).astype(jnp.bfloat16)
        for p in range(ntp):
            att[p, :, t * LANES : (t + 1) * LANES] = done[p * share : (p + 1) * share]

    def across(d):
        to = (tp + d) % ntp
        return pltpu.make_async_remote_copy(
            src_ref=att.at[to], dst_ref=rx.at[tp],
            send_sem=send_t.at[d], recv_sem=recv_t.at[d],
            device_id=(sp, to), device_id_type=MESH,
        )

    for d in range(1, ntp):
        across(d).start()
    rx[tp] = att[tp]
    for i in range(steps):
        forward(i).wait_send()
        backward(i).wait_send()
    for d in range(1, ntp):
        across(d).wait_recv()
    width = q_ref.shape[1]
    for p in range(ntp):
        out_ref[:, p * width : (p + 1) * width] = rx[p]
    for d in range(1, ntp):
        across(d).wait_send()


def ring_sizes(mesh, n):
    try:
        coords = [tuple(d.coords) for d in mesh.devices[:, 0]]
        nz = len({c[2] for c in coords})
        nx = len({c[0] for c in coords})
        if nz * nx == n and nz > 1:
            return nz, nx
    except Exception:
        pass
    return n, 1


def attend(mesh, query_proj, projected_keys, projected_values):
    n, ntp = mesh.shape["sp"], mesh.shape["tp"]
    nz, nx = ring_sizes(mesh, n)
    toks, width = query_proj.shape
    heads = width // HEAD_SIZE
    group = heads // (projected_keys.shape[1] // HEAD_SIZE)
    spare = LANES - projected_keys.shape[1]
    if spare:
        projected_keys = jnp.pad(projected_keys, ((0, 0), (0, spare)))
        projected_values = jnp.pad(projected_values, ((0, 0), (0, spare)))
    quarter = HEAD_SIZE // 4
    places = lax.axis_index("sp") * toks + jnp.arange(toks, dtype=jnp.int32)
    frequency = base_theta ** (-jnp.arange(quarter, dtype=jnp.float32) / quarter)
    lane = jnp.arange(LANES, dtype=jnp.int32)
    on_row = (lane % HEAD_SIZE) < 2 * quarter
    spot = jnp.where(on_row[None, :], (places // GRID_W)[:, None], (places % GRID_W)[:, None])
    angle = spot.astype(jnp.float32) * jnp.tile(frequency, LANES // quarter)[None, :]
    first = (lane // quarter) % 2 == 0
    source = jnp.where(first, lane + quarter, lane - quarter)
    swap = jnp.where(
        lane[:, None] == source[None, :], jnp.where(first, -1.0, 1.0)[None, :], 0.0
    ).astype(jnp.bfloat16)
    ones = jnp.where(
        lane[:, None] // HEAD_SIZE == lane[None, :] // HEAD_SIZE, 1.0 / HEAD_SIZE, 0.0
    ).astype(jnp.bfloat16)
    share = toks // ntp
    dma = pltpu.SemaphoreType.DMA
    return pl.pallas_call(
        functools.partial(attend_kernel, n, nz, nx, ntp, group),
        out_shape=jax.ShapeDtypeStruct((share, ntp * width), jnp.bfloat16),
        in_specs=[pl.BlockSpec(memory_space=pltpu.HBM)] * 3
        + [pl.BlockSpec(memory_space=pltpu.VMEM)] * 4,
        out_specs=pl.BlockSpec(memory_space=pltpu.VMEM),
        scratch_shapes=[
            pltpu.VMEM(query_proj.shape, jnp.bfloat16),
            pltpu.VMEM(projected_keys.shape, jnp.bfloat16),
            pltpu.VMEM(projected_keys.shape, jnp.bfloat16),
            pltpu.VMEM((heads * toks, LANES), jnp.bfloat16),
            pltpu.VMEM((heads * toks, LANES), jnp.float32),
            pltpu.VMEM((n + 1, 2, toks // 2, LANES), jnp.bfloat16),
            pltpu.VMEM((n + 1, 2, toks // 2, LANES), jnp.bfloat16),
            pltpu.VMEM((ntp, share, width), jnp.bfloat16),
            pltpu.VMEM((ntp, share, width), jnp.bfloat16),
            dma((3,)),
            dma((n - 1,)), dma((n - 1,)), dma((n - 1,)), dma((n - 1,)),
            dma((ntp,)), dma((ntp,)),
        ],
        compiler_params=pltpu.CompilerParams(
            collective_id=0, has_side_effects=True, vmem_limit_bytes=40 << 20
        ),
        name="attend",
    )(query_proj, projected_keys, projected_values, jnp.cos(angle), jnp.sin(angle), swap, ones)


def moe_kernel(
    count, ntp, cap,
    tx, stream, pick, share_w, gate_hbm, up_hbm, down_hbm,
    out_ref,
    rx, res, ret, act, gate, up, down,
    send_o, recv_o, send_r, recv_r, wsem,
):
    me = lax.axis_index("sp") * ntp + lax.axis_index("tp")
    per = count // 4
    order = (2, 1, 3, 0)

    def device(offset):
        other = (me + offset + count) % count
        return (other // ntp, other % ntp)

    def block(d):
        return pl.ds(pl.multiple_of(d * cap, cap), cap)

    def dispatch(d):
        return pltpu.make_async_remote_copy(
            src_ref=tx.at[block(d)], dst_ref=rx.at[block(d)],
            send_sem=send_o.at[d], recv_sem=recv_o.at[d],
            device_id=device(d), device_id_type=MESH,
        )

    def answer(d):
        return pltpu.make_async_remote_copy(
            src_ref=res.at[block(d)], dst_ref=ret.at[block(d)],
            send_sem=send_r.at[d], recv_sem=recv_r.at[d],
            device_id=device(-d), device_id_type=MESH,
        )

    def each(first, last, action):
        def body(d, carry):
            action(d)
            return carry

        lax.fori_loop(max(first, 1), last, body, 0)

    barrier = pltpu.get_barrier_semaphore()
    each(1, count, lambda d: pl.semaphore_signal(
        barrier, inc=1, device_id=device(d), device_id_type=MESH
    ))
    loads = [
        pltpu.make_async_copy(gate_hbm.at[0], gate, wsem.at[0]),
        pltpu.make_async_copy(up_hbm.at[0], up, wsem.at[1]),
        pltpu.make_async_copy(down_hbm.at[0], down, wsem.at[2]),
    ]
    pl.semaphore_wait(barrier, count - 1)
    for g in order:
        each(g * per, (g + 1) * per, lambda d: dispatch(d).start())
    for load in loads:
        load.start()
    rx[0:cap] = tx[0:cap]

    def columns(total, body):
        tile = math.gcd(total, 256)

        def one(c, carry):
            body(pl.ds(pl.multiple_of(c * tile, tile), tile))
            return carry

        lax.fori_loop(0, total // tile, one, 0)

    for number, g in enumerate(order):
        each(g * per, (g + 1) * per, lambda d: dispatch(d).wait_recv())
        if number == 0:
            for load in loads:
                load.wait()
        rows = slice(g * per * cap, (g + 1) * per * cap)

        def hidden(cols):
            taken = rx[rows]
            pre = jnp.dot(taken, gate[:, cols], preferred_element_type=jnp.float32)
            lift = jnp.dot(taken, up[:, cols], preferred_element_type=jnp.float32)
            act[:, cols] = (pre / (1.0 + jnp.exp(-pre)) * lift).astype(jnp.bfloat16)

        def project(cols):
            res[rows, cols] = jnp.dot(
                act[...], down[:, cols], preferred_element_type=jnp.float32
            ).astype(jnp.bfloat16)

        columns(gate.shape[1], hidden)
        columns(down.shape[1], project)
        each(g * per, (g + 1) * per, lambda d: answer(d).start())
    ret[0:cap] = res[0:cap]
    each(1, count, lambda d: answer(d).wait_recv())

    def combine(cols):
        total = jnp.zeros((out_ref.shape[0], math.gcd(out_ref.shape[1], 256)), jnp.float32)
        for k in range(pick.shape[0]):
            total += share_w[:, k : k + 1] * jnp.dot(
                pick[k], ret[:, cols], preferred_element_type=jnp.float32
            )
        out_ref[:, cols] = (stream[:, cols].astype(jnp.float32) + total).astype(jnp.bfloat16)

    columns(out_ref.shape[1], combine)
    each(1, count, lambda d: dispatch(d).wait_send())
    each(1, count, lambda d: answer(d).wait_send())


def moe(mesh, cap, outgoing, stream, pick, share_w, expert_gate, expert_up, expert_down):
    ntp = mesh.shape["tp"]
    count = mesh.shape["sp"] * ntp
    width = outgoing.shape[1]
    ff = expert_gate.shape[2]
    dma = pltpu.SemaphoreType.DMA
    low = jnp.bfloat16
    return pl.pallas_call(
        functools.partial(moe_kernel, count, ntp, cap),
        out_shape=jax.ShapeDtypeStruct(stream.shape, low),
        in_specs=[pl.BlockSpec(memory_space=pltpu.VMEM)] * 4
        + [pl.BlockSpec(memory_space=pl.ANY)] * 3,
        out_specs=pl.BlockSpec(memory_space=pltpu.VMEM),
        scratch_shapes=[
            pltpu.VMEM((count * cap, width), low),
            pltpu.VMEM((count * cap, width), low),
            pltpu.VMEM((count * cap, width), low),
            pltpu.VMEM((count // 4 * cap, ff), low),
            pltpu.VMEM((width, ff), low),
            pltpu.VMEM((width, ff), low),
            pltpu.VMEM((ff, width), low),
            dma((count,)), dma((count,)), dma((count,)), dma((count,)), dma((3,)),
        ],
        compiler_params=pltpu.CompilerParams(
            collective_id=1, has_side_effects=True, vmem_limit_bytes=60 << 20
        ),
        name="moe",
    )(outgoing, stream, pick, share_w, expert_gate, expert_up, expert_down)


def local(
    mesh,
    query_proj,
    projected_keys,
    projected_values,
    residual,
    out_weight,
    mix_gain,
    norm_gain,
    route_expert,
    route_weight,
    expert_gate,
    expert_up,
    expert_down,
):
    by_token = attend(mesh, query_proj, projected_keys, projected_values)
    mixed = jnp.dot(by_token, out_weight, preferred_element_type=jnp.float32)
    stream = (residual.astype(jnp.float32) + unit_length_rows(mixed) * mix_gain).astype(
        jnp.bfloat16
    )
    normed = (unit_length_rows(stream) * norm_gain).astype(jnp.bfloat16)
    row_count = normed.shape[0]
    top_count = route_expert.shape[1]
    experts = lax.axis_size("sp") * lax.axis_size("tp")
    capacity = -(-max(2, 2 * top_count * row_count // experts) // 16) * 16
    flat_expert = route_expert.reshape(-1)
    onehot = (flat_expert[:, None] == jnp.arange(experts, dtype=jnp.int32)[None, :]).astype(
        jnp.int32
    )
    earlier = jnp.cumsum(onehot, axis=0) - onehot
    slot_rank = jnp.sum(earlier * onehot, axis=1)
    me = lax.axis_index("sp") * lax.axis_size("tp") + lax.axis_index("tp")
    target = ((flat_expert - me + experts) % experts) * capacity + slot_rank
    placing = jnp.arange(experts * capacity, dtype=jnp.int32)[:, None] == target[None, :]
    placing = jnp.any(placing.reshape(experts * capacity, row_count, top_count), axis=2).astype(
        jnp.bfloat16
    )
    outgoing = jnp.dot(placing, normed, preferred_element_type=jnp.float32).astype(jnp.bfloat16)
    places = jnp.arange(experts * capacity, dtype=jnp.int32)
    pick = target.reshape(row_count, top_count).T[:, :, None] == places
    return moe(
        mesh, capacity, outgoing, stream, pick.astype(jnp.bfloat16), route_weight,
        expert_gate, expert_up, expert_down,
    )


def solution(mesh):
    return jax.shard_map(
        functools.partial(local, mesh),
        mesh=mesh,
        in_specs=(
            P("sp", "tp"),
            P("sp", "tp"),
            P("sp", "tp"),
            P(("sp", "tp"), None),
            P(),
            P(),
            P(),
            P(("sp", "tp"), None),
            P(("sp", "tp"), None),
            P(("sp", "tp"), None, None),
            P(("sp", "tp"), None, None),
            P(("sp", "tp"), None, None),
        ),
        out_specs=P(("sp", "tp"), None),
        check_vma=False,
    )
```
